32 devices in a mesh: sp: 16 (over z, y, x), tp: 2 (over core).
Axes of the slice: x: 2, y: 2, z: 4, core: 2. Of those that a mesh axis runs over, the one named last changes fastest.
Arguments:
- tokens: bfloat16 [2048, 4096], P('sp'), may hold values from -6 to 6
- norm_gain: float32 [4096], replicated, may hold values from 0.1 to 1.9
- w_query: bfloat16 [4096, 2048], P('sp', 'tp'), may hold values from -1 to 1
- w_key: bfloat16 [4096, 512], P('sp', 'tp'), may hold values from -1 to 1
- w_value: bfloat16 [4096, 512], P('sp', 'tp'), may hold values from -0.09375 to 0.09375
- w_state_in: bfloat16 [4096, 2048], P('sp', 'tp'), may hold values from -0.09375 to 0.09375
- sink_logit: float32 [32], P('tp'), may hold values from 2 to 6
- decay_rate: float32 [128, 64], P('tp'), may hold values from 0.0002 to 4
- rotation: float32 [128, 64], P('tp'), may hold values from 1 to 60
- log_step: float32 [128], P('tp'), may hold values from -5.3 to -3
- in_re: float32 [128, 64, 16], P('tp'), may hold values from -1.5 to 1.5
- in_im: float32 [128, 64, 16], P('tp'), may hold values from -1.5 to 1.5
- out_re: float32 [128, 16, 64], P('tp'), may hold values from -0.75 to 0.75
- out_im: float32 [128, 16, 64], P('tp'), may hold values from -0.75 to 0.75
- skip_gain: float32 [2048], P('tp'), may hold values from -4 to 4
- w_attn_out: bfloat16 [2048, 4096], P('tp', 'sp'), may hold values from -0.5 to 0.5
- w_state_out: bfloat16 [2048, 4096], P('tp', 'sp'), may hold values from -0.125 to 0.125
- out_gain: float32 [4096], replicated, may hold values from 0.1 to 1.9
Outputs:
- mixed: bfloat16 [2048, 4096], P(('sp', 'tp'))
The draws below stay inside these ranges and needn't reach their ends.
All inputs are finite; a program needn't handle non-finite values.
Results may differ from the reference program's by a relative error of at most 0.015.
The reference program's roundings to bfloat16 on the way count: a program that leaves them out, or rounds other values in their place, can miss the bound.
Values may be sent and summed in bfloat16 or wider, within the bound.
No kernel may reach another device: no remote copies, remote signals or barrier semaphores. Data moves between devices by JAX's collectives and lax.ppermute only.
A program may use at most 128 MiB of HBM per device.

```python
import math
import jax
import jax.numpy as jnp
from jax import lax

D = 4096
QH = 32
KVH = 8
HEAD = 64
GSIZE = 16
STATE = 64
WINDOW = 128
TOK_DEV = 128
ATTN = 2048
GROUPS = 128
TOKENS = 2048
N_SP = 16
N_TP = 2


def spiked_columns(key, salt, column_count):
    noise_part = jax.random.normal(jax.random.fold_in(key, salt), (D, column_count), jnp.float32) * D ** (-0.5)
    noise_part = jnp.clip(noise_part, -6.0 * D ** (-0.5), 6.0 * D ** (-0.5))
    return jnp.clip(noise_part, -1.0, 1.0)


def draw_w_query(key, part):
    return spiked_columns(key, 1, QH * HEAD).astype(jnp.bfloat16)


def draw_w_key(key, part):
    return spiked_columns(key, 2, KVH * HEAD).astype(jnp.bfloat16)


def draw_decay_rate(key, part):
    slow_rate = jnp.exp(jax.random.uniform(jax.random.fold_in(key, 11), (GROUPS, STATE), jnp.float32, math.log(0.0002), math.log(0.002)))
    fast_rate = jnp.exp(jax.random.uniform(jax.random.fold_in(key, 12), (GROUPS, STATE), jnp.float32, math.log(2.0), math.log(4.0)))
    picks = jax.random.randint(jax.random.fold_in(key, 13), (GROUPS, 1), 0, 10)
    slow_flag = picks < 5
    return jnp.where(slow_flag, slow_rate, fast_rate)


def levels(key, shape, pieces, smallest, top_value):
    gain = 1.0
    for axis_at, shards_of in pieces:
        heights = jax.random.uniform(jax.random.fold_in(jax.random.fold_in(key, 6), axis_at), (shards_of,), jnp.float32, smallest / len(pieces), top_value / len(pieces))
        gain = gain * jnp.repeat(jnp.exp(heights), shape[axis_at] // shards_of).reshape((-1,) + (1,) * (len(shape) - 1 - axis_at))
    return gain


def noise(key, dims, spread, bound, pieces=(), held_as=jnp.bfloat16):
    values = jax.random.normal(key, dims, jnp.float32) * spread
    if len(pieces) > 0:
        values = levels(key, dims, pieces, -0.22, 0.18) * values
    return jnp.clip(values, min=-bound, max=bound).astype(held_as)


def setup_inputs(seed: int = 0) -> dict:
    key_of = jax.random.split(jax.random.key(seed), 19)
    tokens = noise(key_of[0], (TOKENS, D), 1.0, 6.0, ((0, 16),))
    norm_gain = jnp.clip(1.0 + 0.18 * jax.random.normal(key_of[1], (D,), jnp.float32), 0.1, 1.9)
    w_query = draw_w_query(jax.random.fold_in(key_of[18], 71), 0)
    w_key = draw_w_key(jax.random.fold_in(key_of[18], 71), 0)
    w_value = noise(key_of[4], (D, KVH * HEAD), D ** -0.5, 0.09375, ((0, 16), (1, 2)))
    w_state_in = noise(key_of[5], (D, ATTN), D ** -0.5, 0.09375, ((0, 16), (1, 2)))
    sink_logit = jnp.clip(2.0 + 4.0 * jax.random.uniform(key_of[6], (QH,), jnp.float32) ** levels(key_of[6], (QH,), ((0, 2),), -0.2, 0.2), 2.0, 6.0)
    decay_rate = draw_decay_rate(jax.random.fold_in(key_of[18], 71), 0)
    rotation = jnp.clip(1.0 + 59.0 * jax.random.uniform(key_of[8], (GROUPS, STATE), jnp.float32) ** levels(key_of[8], (GROUPS, STATE), ((0, 2),), -0.2, 0.2), 1.0, 60.0)
    log_step = jnp.clip(-5.3 + 2.3000002 * jax.random.uniform(key_of[9], (GROUPS,), jnp.float32) ** levels(key_of[9], (GROUPS,), ((0, 2),), -0.2, 0.2), -5.3, -3.0)
    in_re = noise(key_of[10], (GROUPS, STATE, GSIZE), GSIZE ** -0.5, 1.5, ((0, 2),), jnp.float32)
    in_im = noise(key_of[11], (GROUPS, STATE, GSIZE), GSIZE ** -0.5, 1.5, ((0, 2),), jnp.float32)
    out_re = noise(key_of[12], (GROUPS, GSIZE, STATE), STATE ** -0.5, 0.75, ((0, 2),), jnp.float32)
    out_im = noise(key_of[13], (GROUPS, GSIZE, STATE), STATE ** -0.5, 0.75, ((0, 2),), jnp.float32)
    skip_gain = noise(key_of[14], (ATTN,), 1.0, 4.0, ((0, 2),), jnp.float32)
    w_attn_out = noise(key_of[15], (ATTN, D), (ATTN // 16) ** -0.5, 0.5, ((0, 2), (1, 16)))
    w_state_out = noise(key_of[16], (ATTN, D), ATTN ** -0.5, 0.125, ((0, 2), (1, 16)))
    out_gain = jnp.clip(1.0 + 0.18 * jax.random.normal(key_of[17], (D,), jnp.float32), 0.1, 1.9)
    return {"tokens": tokens, "norm_gain": norm_gain, "w_query": w_query, "w_key": w_key, "w_value": w_value, "w_state_in": w_state_in, "sink_logit": sink_logit, "decay_rate": decay_rate, "rotation": rotation, "log_step": log_step, "in_re": in_re, "in_im": in_im, "out_re": out_re, "out_im": out_im, "skip_gain": skip_gain, "w_attn_out": w_attn_out, "w_state_out": w_state_out, "out_gain": out_gain}


epsilon = 1e-06
rotary_base = 500000.0

def rotate(heads_block, positions):
    head_width = heads_block.shape[-1]
    half_width = head_width // 2
    frequency = rotary_base ** (-(jnp.arange(half_width, dtype=jnp.float32) * 2.0 / head_width))
    angles = positions.astype(jnp.float32)[:, None] * frequency[None, :]
    cosine = jnp.cos(angles)[:, None, :]
    sine_part = jnp.sin(angles)[:, None, :]
    lower_half = heads_block[..., :half_width]
    upper_half = heads_block[..., half_width:]
    return jnp.concatenate([lower_half * cosine - upper_half * sine_part, upper_half * cosine + lower_half * sine_part], axis=-1)

def shape_heads(query_sum, key_sum, value_sum, positions, head_width):
    row_count = query_sum.shape[0]
    kv_heads = key_sum.shape[1] // head_width
    group_size = query_sum.shape[1] // key_sum.shape[1]
    queries = rotate(query_sum.reshape(row_count, kv_heads * group_size, head_width), positions).astype(jnp.bfloat16)
    queries = queries.reshape(row_count, kv_heads, group_size, head_width)
    key_rows = rotate(key_sum.reshape(row_count, kv_heads, head_width), positions).astype(jnp.bfloat16)
    key_rows = key_rows.reshape(row_count, kv_heads * head_width)
    value_rows = value_sum.astype(jnp.bfloat16)
    return (queries, key_rows, value_rows)

def band_attention(queries, key_rows, value_rows, sink_logit, first_row, window):
    row_count, kv_heads, group_size, head_width = queries.shape
    blocks = row_count // window
    query_blocks = queries.reshape(blocks, window, kv_heads, group_size, head_width).astype(jnp.float32)
    key_blocks = jnp.concatenate([key_rows[:row_count].reshape(blocks, window, kv_heads, head_width), key_rows[window:].reshape(blocks, window, kv_heads, head_width)], axis=1)
    value_blocks = jnp.concatenate([value_rows[:row_count].reshape(blocks, window, kv_heads, head_width), value_rows[window:].reshape(blocks, window, kv_heads, head_width)], axis=1)
    scores = jnp.einsum('bqkgd,bskd->bkgqs', query_blocks, key_blocks.astype(jnp.float32)) / math.sqrt(head_width)
    block_start = jnp.arange(blocks, dtype=jnp.int32)[:, None, None] * window
    query_at = first_row + block_start + jnp.arange(window, dtype=jnp.int32)[None, :, None]
    key_at = first_row - window + block_start + jnp.arange(2 * window, dtype=jnp.int32)[None, None, :]
    offset_gap = query_at - key_at
    visible = (offset_gap >= 0) & (offset_gap < window) & (key_at >= 0)
    scores = jnp.where(visible[:, None, None, :, :], scores, -jnp.inf)
    sink_value = sink_logit.astype(jnp.float32).reshape(1, kv_heads, group_size, 1, 1)
    top_score = jnp.maximum(lax.optimization_barrier(jnp.max(scores, axis=-1, keepdims=True)), sink_value)
    exponent = jnp.exp(scores - top_score)
    totals = lax.optimization_barrier(jnp.sum(exponent, axis=-1, keepdims=True)) + jnp.exp(sink_value - top_score)
    weights = (exponent / totals).astype(jnp.bfloat16)
    attended = jnp.einsum('bkgqs,bskd->bqkgd', weights.astype(jnp.float32), value_blocks.astype(jnp.float32))
    return attended.reshape(row_count, kv_heads * group_size * head_width).astype(jnp.bfloat16)

def discretize(decay_rate, rotation, log_step, in_re, in_im):
    time_step = jnp.exp(log_step)[:, None]
    lambda_re = -decay_rate
    lambda_im = rotation
    modulus = jnp.exp(lambda_re * time_step)
    pole_re = modulus * jnp.cos(lambda_im * time_step)
    pole_im = modulus * jnp.sin(lambda_im * time_step)
    minus_one = pole_re - 1.0
    denominator = lambda_re * lambda_re + lambda_im * lambda_im
    factor_re = ((minus_one * lambda_re + pole_im * lambda_im) / denominator)[..., None]
    factor_im = ((pole_im * lambda_re - minus_one * lambda_im) / denominator)[..., None]
    drive_re = factor_re * in_re - factor_im * in_im
    drive_im = factor_re * in_im + factor_im * in_re
    return (pole_re, pole_im, drive_re, drive_im)

def chain_link(earlier, later):
    early_are, early_aim, early_bre, early_bim = earlier
    late_are, late_aim, late_bre, late_bim = later
    return (late_are * early_are - late_aim * early_aim, late_are * early_aim + late_aim * early_are, late_are * early_bre - late_aim * early_bim + late_bre, late_are * early_bim + late_aim * early_bre + late_bim)

def local_states(inputs, pole_re, pole_im, drive_re, drive_im):
    row_count = inputs.shape[0]
    groups, states, group_width = drive_re.shape
    channel_values = inputs.astype(jnp.float32).reshape(row_count, groups, group_width)
    push_re = jnp.einsum('tgh,gph->tgp', channel_values, drive_re, precision=lax.Precision.HIGHEST).reshape(row_count, groups * states)
    push_im = jnp.einsum('tgh,gph->tgp', channel_values, drive_im, precision=lax.Precision.HIGHEST).reshape(row_count, groups * states)
    decay_re = jnp.broadcast_to(pole_re.reshape(1, groups * states), push_re.shape)
    decay_im = jnp.broadcast_to(pole_im.reshape(1, groups * states), push_im.shape)
    return lax.associative_scan(chain_link, (decay_re, decay_im, push_re, push_im), axis=0)

def apply_carry(running, carry_re, carry_im):
    power_re, power_im, own_re, own_im = running
    return (own_re + power_re * carry_re - power_im * carry_im, own_im + power_re * carry_im + power_im * carry_re)

def read_out(inputs, state_re, state_im, out_re, out_im, skip_gain):
    row_count = inputs.shape[0]
    groups, group_width, states = out_re.shape
    grid_re = state_re.reshape(row_count, groups, states)
    grid_im = state_im.reshape(row_count, groups, states)
    summed = jnp.einsum('tgp,ghp->tgh', grid_re, out_re, precision=lax.Precision.HIGHEST) - jnp.einsum('tgp,ghp->tgh', grid_im, out_im, precision=lax.Precision.HIGHEST)
    summed = summed.reshape(row_count, groups * group_width) + skip_gain * inputs.astype(jnp.float32)
    return jax.nn.gelu(summed).astype(jnp.bfloat16)

def reference(tokens, norm_gain, w_query, w_key, w_value, w_state_in, sink_logit, decay_rate, rotation, log_step, in_re, in_im, out_re, out_im, skip_gain, w_attn_out, w_state_out, out_gain):
    wide_tokens = tokens.astype(jnp.float32)
    normed = (wide_tokens * lax.rsqrt(lax.optimization_barrier(jnp.mean(wide_tokens * wide_tokens, axis=-1, keepdims=True)) + epsilon) * norm_gain).astype(jnp.bfloat16)
    positions = jnp.arange(TOKENS, dtype=jnp.int32)
    query_sum = jnp.dot(normed, w_query, preferred_element_type=jnp.float32)
    key_sum = jnp.dot(normed, w_key, preferred_element_type=jnp.float32)
    value_sum = jnp.dot(normed, w_value, preferred_element_type=jnp.float32)
    queries, key_rows, value_rows = shape_heads(query_sum, key_sum, value_sum, positions, HEAD)
    inputs = jnp.dot(normed, w_state_in, preferred_element_type=jnp.float32).astype(jnp.bfloat16)
    padded_keys = jnp.concatenate([jnp.zeros((WINDOW, KVH * HEAD), jnp.bfloat16), key_rows], axis=0)
    padded_values = jnp.concatenate([jnp.zeros((WINDOW, KVH * HEAD), jnp.bfloat16), value_rows], axis=0)

    def span_attend(span_index):
        first_row = (span_index * TOK_DEV).astype(jnp.int32)
        span_queries = lax.dynamic_slice_in_dim(queries, first_row, TOK_DEV, 0)
        span_keys = lax.dynamic_slice_in_dim(padded_keys, first_row, TOK_DEV + WINDOW, 0).reshape(TOK_DEV + WINDOW, KVH, HEAD)
        span_values = lax.dynamic_slice_in_dim(padded_values, first_row, TOK_DEV + WINDOW, 0).reshape(TOK_DEV + WINDOW, KVH, HEAD)
        return band_attention(span_queries, span_keys, span_values, sink_logit, first_row, WINDOW)
    attended = lax.map(span_attend, jnp.arange(N_SP, dtype=jnp.int32)).reshape(TOKENS, ATTN)
    pole_re, pole_im, drive_re, drive_im = discretize(decay_rate, rotation, log_step, in_re, in_im)
    spans = inputs.reshape(N_SP, TOK_DEV, ATTN)

    def span_step(carried, span_inputs):
        running = local_states(span_inputs, pole_re, pole_im, drive_re, drive_im)
        state_re, state_im = apply_carry(running, carried[0], carried[1])
        out_rows = read_out(span_inputs, state_re, state_im, out_re, out_im, skip_gain)
        return ((state_re[-1], state_im[-1]), out_rows)
    start_state = (jnp.zeros((GROUPS * STATE,), jnp.float32), jnp.zeros((GROUPS * STATE,), jnp.float32))
    final_state, mixed_spans = lax.scan(span_step, start_state, spans)
    mixed_state = mixed_spans.reshape(TOKENS, ATTN)
    block_width = ATTN // N_TP
    projected = jnp.zeros((TOKENS, D), jnp.float32)
    for block_index in range(N_TP):
        low = block_index * block_width
        partial_term = jnp.dot(attended[:, low:low + block_width], w_attn_out[low:low + block_width], preferred_element_type=jnp.float32) + jnp.dot(mixed_state[:, low:low + block_width], w_state_out[low:low + block_width], preferred_element_type=jnp.float32)
        rounded = lax.optimization_barrier(partial_term.astype(jnp.bfloat16))
        projected = projected + rounded.astype(jnp.float32)
    row_scale = lax.rsqrt(lax.optimization_barrier(jnp.mean(projected * projected, axis=-1, keepdims=True)) + epsilon)
    return (projected * row_scale * out_gain).astype(jnp.bfloat16)
```

```python
import math

import jax
import jax.numpy as jnp
from jax import lax
from jax.experimental import pallas as pl
from jax.experimental.pallas import tpu as pltpu
from jax.sharding import PartitionSpec as P

HEAD = 64
WINDOW = 128


epsilon = 1e-06
rotary_base = 500000.0


def passed_along(value, axis, by):
    size = lax.axis_size(axis)
    pairs = [(i, i + by) for i in range(size) if 0 <= i + by < size]
    return lax.ppermute(value, axis, pairs)


def rotate(heads_block, positions):
    head_width = heads_block.shape[-1]
    half_width = head_width // 2
    frequency = rotary_base ** (-(jnp.arange(half_width, dtype=jnp.float32) * 2.0 / head_width))
    angles = positions.astype(jnp.float32)[:, None] * frequency[None, :]
    cosine = jnp.cos(angles)[:, None, :]
    sine_part = jnp.sin(angles)[:, None, :]
    lower_half = heads_block[..., :half_width]
    upper_half = heads_block[..., half_width:]
    return jnp.concatenate(
        [
            lower_half * cosine - upper_half * sine_part,
            upper_half * cosine + lower_half * sine_part,
        ],
        axis=-1,
    )


def shape_heads(query_sum, key_sum, value_sum, positions, head_width):
    row_count = query_sum.shape[0]
    kv_heads = key_sum.shape[1] // head_width
    group_size = query_sum.shape[1] // key_sum.shape[1]
    queries = rotate(
        query_sum.reshape(row_count, kv_heads * group_size, head_width), positions
    ).astype(jnp.bfloat16)
    queries = queries.reshape(row_count, kv_heads, group_size, head_width)
    key_rows = rotate(key_sum.reshape(row_count, kv_heads, head_width), positions).astype(
        jnp.bfloat16
    )
    key_rows = key_rows.reshape(row_count, kv_heads * head_width)
    value_rows = value_sum.astype(jnp.bfloat16)
    return (queries, key_rows, value_rows)


def band_attention(queries, key_rows, value_rows, sink_logit, first_row, window):
    row_count, kv_heads, group_size, head_width = queries.shape
    blocks = row_count // window
    query_blocks = queries.reshape(blocks, window, kv_heads, group_size, head_width)
    key_blocks = jnp.concatenate(
        [
            key_rows[:row_count].reshape(blocks, window, kv_heads, head_width),
            key_rows[window:].reshape(blocks, window, kv_heads, head_width),
        ],
        axis=1,
    )
    value_blocks = jnp.concatenate(
        [
            value_rows[:row_count].reshape(blocks, window, kv_heads, head_width),
            value_rows[window:].reshape(blocks, window, kv_heads, head_width),
        ],
        axis=1,
    )
    scores = jnp.einsum(
        "bqkgd,bskd->bkgqs", query_blocks, key_blocks, preferred_element_type=jnp.float32
    ) / math.sqrt(head_width)
    block_start = jnp.arange(blocks, dtype=jnp.int32)[:, None, None] * window
    query_at = first_row + block_start + jnp.arange(window, dtype=jnp.int32)[None, :, None]
    key_at = (
        first_row - window + block_start + jnp.arange(2 * window, dtype=jnp.int32)[None, None, :]
    )
    offset_gap = query_at - key_at
    visible = (offset_gap >= 0) & (offset_gap < window) & (key_at >= 0)
    scores = jnp.where(visible[:, None, None, :, :], scores, -jnp.inf)
    sink_value = sink_logit.reshape(1, kv_heads, group_size, 1, 1)
    top_score = jnp.maximum(jnp.max(scores, axis=-1, keepdims=True), sink_value)
    exponent = jnp.exp(scores - top_score)
    totals = jnp.sum(exponent, axis=-1, keepdims=True) + jnp.exp(sink_value - top_score)
    weights = (exponent / totals).astype(jnp.bfloat16)
    attended = jnp.einsum(
        "bkgqs,bskd->bqkgd", weights, value_blocks, preferred_element_type=jnp.float32
    )
    return attended.reshape(row_count, kv_heads * group_size * head_width).astype(jnp.bfloat16)


def discretize(decay_rate, rotation, log_step, in_re, in_im):
    time_step = jnp.exp(log_step)[:, None]
    lambda_re = -decay_rate
    modulus = jnp.exp(lambda_re * time_step)
    pole_re = modulus * jnp.cos(rotation * time_step)
    pole_im = modulus * jnp.sin(rotation * time_step)
    minus_one = pole_re - 1.0
    denominator = lambda_re * lambda_re + rotation * rotation
    factor_re = ((minus_one * lambda_re + pole_im * rotation) / denominator)[..., None]
    factor_im = ((pole_im * lambda_re - minus_one * rotation) / denominator)[..., None]
    drive_re = factor_re * in_re - factor_im * in_im
    drive_im = factor_re * in_im + factor_im * in_re
    return (pole_re, pole_im, drive_re, drive_im)


def split_halves(value):
    high = value.astype(jnp.bfloat16)
    low = (value - high.astype(jnp.float32)).astype(jnp.bfloat16)
    return (high, low)


def dot_f32(left, right, contract):
    return lax.dot_general(
        left, right, ((contract), ((), ())), preferred_element_type=jnp.float32
    )


def complex_mul(a_re, a_im, b_re, b_im):
    return (a_re * b_re - a_im * b_im, a_re * b_im + a_im * b_re)


def pushes(inputs, drive):
    drive_high, drive_low = split_halves(drive)
    pushed = dot_f32(inputs, drive_high, ((1,), (0,))) + dot_f32(inputs, drive_low, ((1,), (0,)))
    half = pushed.shape[1] // 2
    return (pushed[:, :half], pushed[:, half:])


def end_kernel(inputs_ref, drive_ref, pole_ref, end_ref):
    re, im = pushes(inputs_ref[...], drive_ref[0])
    rows = re.shape[0]
    powers = [(pole_ref[0, 0:1, :], pole_ref[0, 1:2, :])]
    while 2 ** len(powers) < rows:
        powers.append(complex_mul(*powers[-1], *powers[-1]))
    size = rows
    for power_re, power_im in reversed(powers):
        size = size // 2
        up_re, up_im = complex_mul(re[:size], im[:size], power_re, power_im)
        re, im = (re[size:] + up_re, im[size:] + up_im)
    end_ref[0, 0:1, :] = re
    end_ref[0, 1:2, :] = im


def shifted(value, by):
    if by % 8 == 0:
        return jnp.concatenate([jnp.zeros_like(value[:by]), value[:-by]], axis=0)
    row = lax.broadcasted_iota(jnp.int32, value.shape, 0)
    return jnp.where(row >= by, pltpu.roll(value, by, 0), 0.0)


def mix_kernel(place_ref, inputs_ref, drive_ref, pole_ref, ends_ref, out_ref, skip_ref, mixed_ref):
    inputs = inputs_ref[...]
    rows = inputs.shape[0]
    re, im = pushes(inputs, drive_ref[0])
    power_re, power_im = (pole_ref[0, 0:1, :], pole_ref[0, 1:2, :])
    far_re, far_im = (power_re, power_im)
    step = 1
    while step < rows:
        far_re, far_im = complex_mul(far_re, far_im, far_re, far_im)
        step = step * 2
    mine = place_ref[0]

    def join(position, carry):
        moved_re, moved_im = complex_mul(carry[0], carry[1], far_re, far_im)
        keep = position < mine
        piece = ends_ref[position, 0]
        return (
            jnp.where(keep, moved_re + piece[0:1], carry[0]),
            jnp.where(keep, moved_im + piece[1:2], carry[1]),
        )

    carry = (jnp.zeros_like(power_re), jnp.zeros_like(power_im))
    for position in range(ends_ref.shape[0] - 1):
        carry = join(position, carry)
    add_re, add_im = complex_mul(carry[0], carry[1], power_re, power_im)
    first = lax.broadcasted_iota(jnp.int32, re.shape, 0) == 0
    re = re + jnp.where(first, add_re, 0.0)
    im = im + jnp.where(first, add_im, 0.0)
    step = 1
    while step < rows:
        move_re, move_im = complex_mul(shifted(re, step), shifted(im, step), power_re, power_im)
        re, im = (re + move_re, im + move_im)
        power_re, power_im = complex_mul(power_re, power_im, power_re, power_im)
        step = step * 2
    state_high, state_low = split_halves(jnp.concatenate([re, im], axis=1))
    out_high, out_low = split_halves(out_ref[0])
    contract = ((1,), (1,))
    summed = (
        dot_f32(state_high, out_high, contract)
        + dot_f32(state_low, out_high, contract)
        + dot_f32(state_high, out_low, contract)
    )
    summed = summed + skip_ref[0] * inputs.astype(jnp.float32)
    mixed_ref[...] = jax.nn.gelu(summed).astype(jnp.bfloat16)


def spread(compact, per_block):
    groups, width, states = compact.shape
    tiled = jnp.tile(
        compact.reshape(groups // per_block, per_block * width, states), (1, 1, per_block)
    )
    row_group = lax.broadcasted_iota(jnp.int32, tiled.shape, 1) // width
    lane_group = lax.broadcasted_iota(jnp.int32, tiled.shape, 2) // states
    return jnp.where(row_group == lane_group, tiled, 0.0)


def state_params(decay_rate, rotation, log_step, in_re, in_im, out_re, out_im):
    groups, states, group_width = in_re.shape
    per_block = math.gcd(groups, 128 // group_width)
    blocks = groups // per_block
    pole_re, pole_im, drive_re, drive_im = discretize(decay_rate, rotation, log_step, in_re, in_im)
    drive = jnp.concatenate(
        [
            spread(jnp.swapaxes(drive_re, 1, 2), per_block),
            spread(jnp.swapaxes(drive_im, 1, 2), per_block),
        ],
        axis=2,
    )
    readout = jnp.concatenate([spread(out_re, per_block), spread(-out_im, per_block)], axis=2)
    poles = jnp.stack(
        [pole_re.reshape(blocks, per_block * states), pole_im.reshape(blocks, per_block * states)],
        axis=1,
    )
    return (poles, drive, readout)


def state_ends(inputs, poles, drive):
    blocks, channels, wide = drive.shape
    rows = inputs.shape[0]
    return pl.pallas_call(
        end_kernel,
        grid=(blocks,),
        in_specs=[
            pl.BlockSpec((rows, channels), lambda b: (0, b)),
            pl.BlockSpec((1, channels, wide), lambda b: (b, 0, 0)),
            pl.BlockSpec((1, 2, wide // 2), lambda b: (b, 0, 0)),
        ],
        out_specs=pl.BlockSpec((1, 2, wide // 2), lambda b: (b, 0, 0)),
        out_shape=jax.ShapeDtypeStruct((blocks, 2, wide // 2), jnp.float32),
    )(inputs, drive, poles)


def state_mix(inputs, poles, drive, readout, ends, skip_gain):
    blocks, channels, wide = drive.shape
    rows = inputs.shape[0]
    place = lax.axis_index("sp").astype(jnp.int32).reshape(1)
    return pl.pallas_call(
        mix_kernel,
        grid=(blocks,),
        in_specs=[
            pl.BlockSpec(memory_space=pltpu.SMEM),
            pl.BlockSpec((rows, channels), lambda b: (0, b)),
            pl.BlockSpec((1, channels, wide), lambda b: (b, 0, 0)),
            pl.BlockSpec((1, 2, wide // 2), lambda b: (b, 0, 0)),
            pl.BlockSpec((ends.shape[0], 1, 2, wide // 2), lambda b: (0, b, 0, 0)),
            pl.BlockSpec((1, channels, wide), lambda b: (b, 0, 0)),
            pl.BlockSpec((1, 1, channels), lambda b: (b, 0, 0)),
        ],
        out_specs=pl.BlockSpec((rows, channels), lambda b: (0, b)),
        out_shape=jax.ShapeDtypeStruct(inputs.shape, jnp.bfloat16),
    )(place, inputs, drive, poles, ends, readout, skip_gain.reshape(blocks, 1, channels))


def flow_kernel(inputs_ref, drive_ref, pole_ref, out_ref, skip_ref, mixed_ref, carry_ref):
    @pl.when(pl.program_id(0) == 0)
    def _():
        carry_ref[...] = jnp.zeros_like(carry_ref)

    inputs = inputs_ref[...]
    rows = inputs.shape[0]
    re, im = pushes(inputs, drive_ref[0])
    power_re, power_im = (pole_ref[0, 0:1, :], pole_ref[0, 1:2, :])
    add_re, add_im = complex_mul(carry_ref[0:1, :], carry_ref[1:2, :], power_re, power_im)
    first = lax.broadcasted_iota(jnp.int32, re.shape, 0) == 0
    re = re + jnp.where(first, add_re, 0.0)
    im = im + jnp.where(first, add_im, 0.0)
    step = 1
    while step < rows:
        move_re, move_im = complex_mul(shifted(re, step), shifted(im, step), power_re, power_im)
        re, im = (re + move_re, im + move_im)
        power_re, power_im = complex_mul(power_re, power_im, power_re, power_im)
        step = step * 2
    carry_ref[0:1, :] = re[rows - 1 :]
    carry_ref[1:2, :] = im[rows - 1 :]
    state_high, state_low = split_halves(jnp.concatenate([re, im], axis=1))
    out_high, out_low = split_halves(out_ref[0])
    contract = ((1,), (1,))
    summed = (
        dot_f32(state_high, out_high, contract)
        + dot_f32(state_low, out_high, contract)
        + dot_f32(state_high, out_low, contract)
    )
    summed = summed + skip_ref[...] * inputs.astype(jnp.float32)
    mixed_ref[...] = jax.nn.gelu(summed).astype(jnp.bfloat16)


def state_flow(inputs, poles, drive, readout, skip_gain, chunk):
    _, channels, wide = drive.shape
    rows = inputs.shape[0]
    return pl.pallas_call(
        flow_kernel,
        grid=(rows // chunk,),
        in_specs=[
            pl.BlockSpec((chunk, channels), lambda t: (t, 0)),
            pl.BlockSpec((1, channels, wide), lambda t: (0, 0, 0)),
            pl.BlockSpec((1, 2, wide // 2), lambda t: (0, 0, 0)),
            pl.BlockSpec((1, channels, wide), lambda t: (0, 0, 0)),
            pl.BlockSpec((1, channels), lambda t: (0, 0)),
        ],
        out_specs=pl.BlockSpec((chunk, channels), lambda t: (t, 0)),
        out_shape=jax.ShapeDtypeStruct(inputs.shape, jnp.bfloat16),
        scratch_shapes=[pltpu.VMEM((2, wide // 2), jnp.float32)],
    )(inputs, drive, poles, readout, skip_gain.reshape(1, channels))


def out_kernel(acts_ref, w_ref, sum_ref):
    cores = w_ref.shape[0]
    total = None
    for core in range(cores):
        rows = jnp.concatenate(
            [acts_ref[at] for at in range(core, acts_ref.shape[0], cores)], axis=1
        )
        piece = dot_f32(rows, w_ref[core], ((1,), (0,)))
        piece = piece.astype(jnp.bfloat16).astype(jnp.float32)
        total = piece if total is None else total + piece
    sum_ref[...] = total.astype(jnp.bfloat16)


def out_project(acts, w_pair):
    devices, rows, width = acts.shape
    cores, depth, columns = w_pair.shape
    block = math.gcd(rows, 256)
    return pl.pallas_call(
        out_kernel,
        grid=(rows // block,),
        in_specs=[
            pl.BlockSpec((devices, block, width), lambda t: (0, t, 0)),
            pl.BlockSpec((cores, depth, columns), lambda t: (0, 0, 0)),
        ],
        out_specs=pl.BlockSpec((block, columns), lambda t: (t, 0)),
        out_shape=jax.ShapeDtypeStruct((rows, columns), jnp.bfloat16),
    )(acts, w_pair)


def own_part(value, axis_name):
    size = value.shape[0] // lax.axis_size(axis_name)
    return lax.dynamic_slice_in_dim(value, lax.axis_index(axis_name) * size, size, 0)


def normalize(tokens, norm_gain):
    wide_tokens = tokens.astype(jnp.float32)
    return (
        wide_tokens
        * lax.rsqrt(jnp.mean(wide_tokens * wide_tokens, axis=-1, keepdims=True) + epsilon)
        * norm_gain
    ).astype(jnp.bfloat16)


def by_heads(
    tokens,
    norm_gain,
    w_query,
    w_key,
    w_value,
    w_state_in,
    sink_logit,
    decay_rate,
    rotation,
    log_step,
    in_re,
    in_im,
    out_re,
    out_im,
    skip_gain,
    w_attn_out,
    w_state_out,
    out_gain,
):
    devices = lax.axis_size("sp")
    row_count = tokens.shape[0]
    everyone = ("sp", "tp")
    normed = lax.all_gather(
        normalize(own_part(tokens, "tp"), norm_gain), everyone, axis=0, tiled=True
    )
    rows = normed.shape[0]
    depth = w_query.shape[0]
    repeats = devices // (w_key.shape[1] // HEAD)

    def per_device(weight):
        return weight.reshape(depth, devices, weight.shape[1] // devices)

    def per_head(weight):
        return jnp.repeat(weight.reshape(depth, -1, HEAD), repeats, axis=1)

    pieces = (per_device(w_query), per_head(w_key), per_head(w_value), per_device(w_state_in))
    key_at = pieces[0].shape[2]
    value_at = key_at + HEAD
    input_at = value_at + HEAD
    parcels = jnp.concatenate(pieces, axis=2).transpose(1, 0, 2)
    w_in = lax.all_to_all(parcels, "sp", split_axis=0, concat_axis=0, tiled=True)
    w_in = w_in.reshape(devices * depth, parcels.shape[2])

    def rows_of(weight):
        return weight.reshape(devices, weight.shape[0] // devices, weight.shape[1])

    w_out = jnp.concatenate([rows_of(w_attn_out), rows_of(w_state_out)], axis=1)
    w_out = w_out.reshape(1, -1, w_out.shape[2])
    w_pair = lax.all_to_all(w_out, "tp", split_axis=2, concat_axis=0, tiled=True)
    decay_rate, rotation, log_step, in_re, in_im, out_re, out_im, skip_gain, sink_logit = [
        own_part(value, "sp")
        for value in (
            decay_rate, rotation, log_step, in_re, in_im, out_re, out_im, skip_gain, sink_logit
        )
    ]
    poles, drive, readout = state_params(
        decay_rate, rotation, log_step, in_re, in_im, out_re, out_im
    )
    sums = jnp.dot(normed, w_in, preferred_element_type=jnp.float32)
    inputs = sums[:, input_at:].astype(jnp.bfloat16)
    queries, key_rows, value_rows = shape_heads(
        sums[:, :key_at],
        sums[:, key_at:value_at],
        sums[:, value_at:input_at],
        jnp.arange(rows, dtype=jnp.int32),
        HEAD,
    )

    def padded(value):
        return jnp.pad(value, ((WINDOW, 0), (0, 0))).reshape(WINDOW + rows, 1, HEAD)

    attended = band_attention(
        queries, padded(key_rows), padded(value_rows), sink_logit, jnp.int32(0), WINDOW
    )
    mixed_state = state_flow(inputs, poles, drive, readout, skip_gain, row_count)
    acts = lax.all_gather(
        jnp.concatenate([attended, mixed_state], axis=1), everyone, axis=0, tiled=False
    )
    summed = out_project(acts, w_pair)
    projected = lax.all_to_all(summed, everyone, split_axis=0, concat_axis=1, tiled=True)
    projected = projected.astype(jnp.float32)
    row_scale = lax.rsqrt(jnp.mean(projected * projected, axis=-1, keepdims=True) + epsilon)
    return (projected * row_scale * out_gain).astype(jnp.bfloat16)


def everyones(value, axis):
    size = lax.axis_size(axis)
    copies = jnp.broadcast_to(value[None], (size,) + value.shape)
    return lax.all_to_all(copies, axis, split_axis=0, concat_axis=0, tiled=True)


def earlier_window(key_rows, value_rows):
    joined = jnp.concatenate([key_rows, value_rows], axis=1)
    prior = passed_along(joined, "sp", 1)
    return jnp.concatenate([prior, joined], axis=0)


def by_tokens(
    tokens,
    norm_gain,
    w_query,
    w_key,
    w_value,
    w_state_in,
    sink_logit,
    decay_rate,
    rotation,
    log_step,
    in_re,
    in_im,
    out_re,
    out_im,
    skip_gain,
    w_attn_out,
    w_state_out,
    out_gain,
):
    row_count = tokens.shape[0]
    window = WINDOW
    head_width = HEAD
    wide_tokens = tokens.astype(jnp.float32)
    normed = (
        wide_tokens
        * lax.rsqrt(jnp.mean(wide_tokens * wide_tokens, axis=-1, keepdims=True) + epsilon)
        * norm_gain
    ).astype(jnp.bfloat16)
    first_row = lax.axis_index("sp") * row_count
    positions = first_row + jnp.arange(row_count, dtype=jnp.int32)
    poles, drive, readout = state_params(
        decay_rate, rotation, log_step, in_re, in_im, out_re, out_im
    )
    slab = lax.all_to_all(normed, "sp", split_axis=1, concat_axis=0, tiled=True)
    w_in = jnp.concatenate([w_query, w_key, w_value, w_state_in], axis=1)
    sums = lax.psum_scatter(
        jnp.dot(slab, w_in, preferred_element_type=jnp.float32).astype(jnp.bfloat16),
        "sp",
        scatter_dimension=0,
        tiled=True,
    )
    key_at = w_query.shape[1]
    value_at = key_at + w_key.shape[1]
    input_at = value_at + w_value.shape[1]
    inputs = sums[:, input_at:]
    ends = everyones(state_ends(inputs, poles, drive), "sp")
    queries, key_rows, value_rows = shape_heads(
        sums[:, :key_at].astype(jnp.float32),
        sums[:, key_at:value_at].astype(jnp.float32),
        sums[:, value_at:input_at],
        positions,
        head_width,
    )
    joined_rows = earlier_window(key_rows, value_rows)
    kv_width = key_rows.shape[1]
    kv_heads = kv_width // head_width
    all_keys = joined_rows[:, :kv_width].reshape(window + row_count, kv_heads, head_width)
    all_values = joined_rows[:, kv_width:].reshape(window + row_count, kv_heads, head_width)
    attended = band_attention(queries, all_keys, all_values, sink_logit, first_row, window)
    mixed_state = state_mix(inputs, poles, drive, readout, ends, skip_gain)
    rows = lax.all_gather(
        jnp.concatenate([attended, mixed_state], axis=1), "sp", axis=0, tiled=True
    )
    w_out = jnp.concatenate([w_attn_out, w_state_out], axis=0)
    partial = jnp.dot(rows, w_out, preferred_element_type=jnp.float32).astype(jnp.bfloat16)
    cores = lax.axis_size("tp")
    blocks = partial.reshape(-1, cores, row_count // cores, partial.shape[1])
    halves = lax.all_to_all(blocks, "tp", split_axis=1, concat_axis=1, tiled=True)
    summed = jnp.sum(halves.astype(jnp.float32), axis=1).astype(jnp.bfloat16)
    projected = lax.all_to_all(summed, "sp", split_axis=0, concat_axis=2, tiled=True)
    projected = projected.reshape(row_count // cores, -1).astype(jnp.float32)
    row_scale = lax.rsqrt(jnp.mean(projected * projected, axis=-1, keepdims=True) + epsilon)
    return (projected * row_scale * out_gain).astype(jnp.bfloat16)


def body(tokens, norm_gain, w_query, w_key, *others):
    devices = lax.axis_size("sp")
    heads = w_query.shape[1] // HEAD
    groups = others[5].shape[0]
    group_size = w_query.shape[1] // w_key.shape[1]
    fits = (
        heads % devices == 0
        and groups % devices == 0
        and group_size % max(heads // devices, 1) == 0
        and tokens.shape[0] % (8 * lax.axis_size("tp")) == 0
    )
    return (by_heads if fits else by_tokens)(tokens, norm_gain, w_query, w_key, *others)


def solution(mesh):
    return jax.shard_map(
        body,
        mesh=mesh,
        in_specs=(
            P("sp", None),
            P(),
            P("sp", "tp"),
            P("sp", "tp"),
            P("sp", "tp"),
            P("sp", "tp"),
            P("tp"),
            P("tp", None),
            P("tp", None),
            P("tp"),
            P("tp", None, None),
            P("tp", None, None),
            P("tp", None, None),
            P("tp", None, None),
            P("tp"),
            P("tp", "sp"),
            P("tp", "sp"),
            P(),
        ),
        out_specs=P(("sp", "tp"), None),
        check_vma=False,
    )
```

```python
import math

import jax
import jax.numpy as jnp
from jax import lax
from jax.experimental import pallas as pl
from jax.experimental.pallas import tpu as pltpu
from jax.sharding import PartitionSpec as P

HEAD = 64
WINDOW = 128


epsilon = 1e-06
rotary_base = 500000.0


def passed_along(value, axis, by):
    size = lax.axis_size(axis)
    pairs = [(i, i + by) for i in range(size) if 0 <= i + by < size]
    return lax.ppermute(value, axis, pairs)


def rotate(heads_block, positions):
    head_width = heads_block.shape[-1]
    half_width = head_width // 2
    frequency = rotary_base ** (-(jnp.arange(half_width, dtype=jnp.float32) * 2.0 / head_width))
    angles = positions.astype(jnp.float32)[:, None] * frequency[None, :]
    cosine = jnp.cos(angles)[:, None, :]
    sine_part = jnp.sin(angles)[:, None, :]
    lower_half = heads_block[..., :half_width]
    upper_half = heads_block[..., half_width:]
    return jnp.concatenate(
        [
            lower_half * cosine - upper_half * sine_part,
            upper_half * cosine + lower_half * sine_part,
        ],
        axis=-1,
    )


def shape_heads(query_sum, key_sum, value_sum, positions, head_width):
    row_count = query_sum.shape[0]
    kv_heads = key_sum.shape[1] // head_width
    group_size = query_sum.shape[1] // key_sum.shape[1]
    queries = rotate(
        query_sum.reshape(row_count, kv_heads * group_size, head_width), positions
    ).astype(jnp.bfloat16)
    queries = queries.reshape(row_count, kv_heads, group_size, head_width)
    key_rows = rotate(key_sum.reshape(row_count, kv_heads, head_width), positions).astype(
        jnp.bfloat16
    )
    key_rows = key_rows.reshape(row_count, kv_heads * head_width)
    value_rows = value_sum.astype(jnp.bfloat16)
    return (queries, key_rows, value_rows)


def band_attention(queries, key_rows, value_rows, sink_logit, first_row, window):
    row_count, kv_heads, group_size, head_width = queries.shape
    blocks = row_count // window
    query_blocks = queries.reshape(blocks, window, kv_heads, group_size, head_width)
    key_blocks = jnp.concatenate(
        [
            key_rows[:row_count].reshape(blocks, window, kv_heads, head_width),
            key_rows[window:].reshape(blocks, window, kv_heads, head_width),
        ],
        axis=1,
    )
    value_blocks = jnp.concatenate(
        [
            value_rows[:row_count].reshape(blocks, window, kv_heads, head_width),
            value_rows[window:].reshape(blocks, window, kv_heads, head_width),
        ],
        axis=1,
    )
    scores = jnp.einsum(
        "bqkgd,bskd->bkgqs", query_blocks, key_blocks, preferred_element_type=jnp.float32
    ) / math.sqrt(head_width)
    block_start = jnp.arange(blocks, dtype=jnp.int32)[:, None, None] * window
    query_at = first_row + block_start + jnp.arange(window, dtype=jnp.int32)[None, :, None]
    key_at = (
        first_row - window + block_start + jnp.arange(2 * window, dtype=jnp.int32)[None, None, :]
    )
    offset_gap = query_at - key_at
    visible = (offset_gap >= 0) & (offset_gap < window) & (key_at >= 0)
    scores = jnp.where(visible[:, None, None, :, :], scores, -jnp.inf)
    sink_value = sink_logit.reshape(1, kv_heads, group_size, 1, 1)
    top_score = jnp.maximum(jnp.max(scores, axis=-1, keepdims=True), sink_value)
    exponent = jnp.exp(scores - top_score)
    totals = jnp.sum(exponent, axis=-1, keepdims=True) + jnp.exp(sink_value - top_score)
    weights = (exponent / totals).astype(jnp.bfloat16)
    attended = jnp.einsum(
        "bkgqs,bskd->bqkgd", weights, value_blocks, preferred_element_type=jnp.float32
    )
    return attended.reshape(row_count, kv_heads * group_size * head_width).astype(jnp.bfloat16)


def discretize(decay_rate, rotation, log_step, in_re, in_im):
    time_step = jnp.exp(log_step)[:, None]
    lambda_re = -decay_rate
    modulus = jnp.exp(lambda_re * time_step)
    pole_re = modulus * jnp.cos(rotation * time_step)
    pole_im = modulus * jnp.sin(rotation * time_step)
    minus_one = pole_re - 1.0
    denominator = lambda_re * lambda_re + rotation * rotation
    factor_re = ((minus_one * lambda_re + pole_im * rotation) / denominator)[..., None]
    factor_im = ((pole_im * lambda_re - minus_one * rotation) / denominator)[..., None]
    drive_re = factor_re * in_re - factor_im * in_im
    drive_im = factor_re * in_im + factor_im * in_re
    return (pole_re, pole_im, drive_re, drive_im)


def split_halves(value):
    high = value.astype(jnp.bfloat16)
    low = (value - high.astype(jnp.float32)).astype(jnp.bfloat16)
    return (high, low)


def dot_f32(left, right, contract):
    return lax.dot_general(
        left, right, ((contract), ((), ())), preferred_element_type=jnp.float32
    )


def complex_mul(a_re, a_im, b_re, b_im):
    return (a_re * b_re - a_im * b_im, a_re * b_im + a_im * b_re)


def pushes(inputs, drive):
    drive_high, drive_low = split_halves(drive)
    pushed = dot_f32(inputs, drive_high, ((1,), (0,))) + dot_f32(inputs, drive_low, ((1,), (0,)))
    half = pushed.shape[1] // 2
    return (pushed[:, :half], pushed[:, half:])


def end_kernel(inputs_ref, drive_ref, pole_ref, end_ref):
    re, im = pushes(inputs_ref[...], drive_ref[0])
    rows = re.shape[0]
    powers = [(pole_ref[0, 0:1, :], pole_ref[0, 1:2, :])]
    while 2 ** len(powers) < rows:
        powers.append(complex_mul(*powers[-1], *powers[-1]))
    size = rows
    for power_re, power_im in reversed(powers):
        size = size // 2
        up_re, up_im = complex_mul(re[:size], im[:size], power_re, power_im)
        re, im = (re[size:] + up_re, im[size:] + up_im)
    end_ref[0, 0:1, :] = re
    end_ref[0, 1:2, :] = im


def shifted(value, by):
    if by % 8 == 0:
        return jnp.concatenate([jnp.zeros_like(value[:by]), value[:-by]], axis=0)
    row = lax.broadcasted_iota(jnp.int32, value.shape, 0)
    return jnp.where(row >= by, pltpu.roll(value, by, 0), 0.0)


def mix_kernel(place_ref, inputs_ref, drive_ref, pole_ref, ends_ref, out_ref, skip_ref, mixed_ref):
    inputs = inputs_ref[...]
    rows = inputs.shape[0]
    re, im = pushes(inputs, drive_ref[0])
    power_re, power_im = (pole_ref[0, 0:1, :], pole_ref[0, 1:2, :])
    far_re, far_im = (power_re, power_im)
    step = 1
    while step < rows:
        far_re, far_im = complex_mul(far_re, far_im, far_re, far_im)
        step = step * 2
    mine = place_ref[0]

    def join(position, carry):
        moved_re, moved_im = complex_mul(carry[0], carry[1], far_re, far_im)
        keep = position < mine
        piece = ends_ref[position, 0]
        return (
            jnp.where(keep, moved_re + piece[0:1], carry[0]),
            jnp.where(keep, moved_im + piece[1:2], carry[1]),
        )

    carry = (jnp.zeros_like(power_re), jnp.zeros_like(power_im))
    for position in range(ends_ref.shape[0] - 1):
        carry = join(position, carry)
    add_re, add_im = complex_mul(carry[0], carry[1], power_re, power_im)
    first = lax.broadcasted_iota(jnp.int32, re.shape, 0) == 0
    re = re + jnp.where(first, add_re, 0.0)
    im = im + jnp.where(first, add_im, 0.0)
    step = 1
    while step < rows:
        move_re, move_im = complex_mul(shifted(re, step), shifted(im, step), power_re, power_im)
        re, im = (re + move_re, im + move_im)
        power_re, power_im = complex_mul(power_re, power_im, power_re, power_im)
        step = step * 2
    state_high, state_low = split_halves(jnp.concatenate([re, im], axis=1))
    out_high, out_low = split_halves(out_ref[0])
    contract = ((1,), (1,))
    summed = (
        dot_f32(state_high, out_high, contract)
        + dot_f32(state_low, out_high, contract)
        + dot_f32(state_high, out_low, contract)
    )
    summed = summed + skip_ref[0] * inputs.astype(jnp.float32)
    mixed_ref[...] = jax.nn.gelu(summed).astype(jnp.bfloat16)


def spread(compact, per_block):
    groups, width, states = compact.shape
    tiled = jnp.tile(
        compact.reshape(groups // per_block, per_block * width, states), (1, 1, per_block)
    )
    row_group = lax.broadcasted_iota(jnp.int32, tiled.shape, 1) // width
    lane_group = lax.broadcasted_iota(jnp.int32, tiled.shape, 2) // states
    return jnp.where(row_group == lane_group, tiled, 0.0)


def state_params(decay_rate, rotation, log_step, in_re, in_im, out_re, out_im):
    groups, states, group_width = in_re.shape
    per_block = math.gcd(groups, 128 // group_width)
    blocks = groups // per_block
    pole_re, pole_im, drive_re, drive_im = discretize(decay_rate, rotation, log_step, in_re, in_im)
    drive = jnp.concatenate(
        [
            spread(jnp.swapaxes(drive_re, 1, 2), per_block),
            spread(jnp.swapaxes(drive_im, 1, 2), per_block),
        ],
        axis=2,
    )
    readout = jnp.concatenate([spread(out_re, per_block), spread(-out_im, per_block)], axis=2)
    poles = jnp.stack(
        [pole_re.reshape(blocks, per_block * states), pole_im.reshape(blocks, per_block * states)],
        axis=1,
    )
    return (poles, drive, readout)


def state_ends(inputs, poles, drive):
    blocks, channels, wide = drive.shape
    rows = inputs.shape[0]
    return pl.pallas_call(
        end_kernel,
        grid=(blocks,),
        in_specs=[
            pl.BlockSpec((rows, channels), lambda b: (0, b)),
            pl.BlockSpec((1, channels, wide), lambda b: (b, 0, 0)),
            pl.BlockSpec((1, 2, wide // 2), lambda b: (b, 0, 0)),
        ],
        out_specs=pl.BlockSpec((1, 2, wide // 2), lambda b: (b, 0, 0)),
        out_shape=jax.ShapeDtypeStruct((blocks, 2, wide // 2), jnp.float32),
    )(inputs, drive, poles)


def state_mix(inputs, poles, drive, readout, ends, skip_gain):
    blocks, channels, wide = drive.shape
    rows = inputs.shape[0]
    place = lax.axis_index("sp").astype(jnp.int32).reshape(1)
    return pl.pallas_call(
        mix_kernel,
        grid=(blocks,),
        in_specs=[
            pl.BlockSpec(memory_space=pltpu.SMEM),
            pl.BlockSpec((rows, channels), lambda b: (0, b)),
            pl.BlockSpec((1, channels, wide), lambda b: (b, 0, 0)),
            pl.BlockSpec((1, 2, wide // 2), lambda b: (b, 0, 0)),
            pl.BlockSpec((ends.shape[0], 1, 2, wide // 2), lambda b: (0, b, 0, 0)),
            pl.BlockSpec((1, channels, wide), lambda b: (b, 0, 0)),
            pl.BlockSpec((1, 1, channels), lambda b: (b, 0, 0)),
        ],
        out_specs=pl.BlockSpec((rows, channels), lambda b: (0, b)),
        out_shape=jax.ShapeDtypeStruct(inputs.shape, jnp.bfloat16),
    )(place, inputs, drive, poles, ends, readout, skip_gain.reshape(blocks, 1, channels))


def attend(queries, keys, values, old_keys, old_values, sink, first):
    rows = queries.shape[0]
    contract = ((1,), (1,))
    scale = 1.0 / math.sqrt(HEAD)
    row = lax.broadcasted_iota(jnp.int32, (rows, rows), 0)
    column = lax.broadcasted_iota(jnp.int32, (rows, rows), 1)
    old_seen = column > row if first is None else (column > row) & jnp.logical_not(first)
    old = jnp.where(old_seen, dot_f32(queries, old_keys, contract) * scale, -jnp.inf)
    new = jnp.where(column <= row, dot_f32(queries, keys, contract) * scale, -jnp.inf)
    top = jnp.max(jnp.maximum(old, new), axis=-1, keepdims=True)
    top = jnp.maximum(top, sink)
    old = jnp.exp(old - top)
    new = jnp.exp(new - top)
    totals = jnp.sum(old + new, axis=-1, keepdims=True) + jnp.exp(sink - top)
    plain = ((1,), (0,))
    return dot_f32((old / totals).astype(jnp.bfloat16), old_values, plain) + dot_f32(
        (new / totals).astype(jnp.bfloat16), values, plain
    )


def layer_kernel(
    sink_ref, normed_ref, w_ref, cosine_ref, sine_ref, drive_ref, pole_ref, out_ref, skip_ref,
    acts_ref, keys_ref, values_ref, carry_ref,
):
    start = pl.program_id(0) == 0

    @pl.when(start)
    def _():
        carry_ref[...] = jnp.zeros_like(carry_ref)
        keys_ref[...] = jnp.zeros_like(keys_ref)
        values_ref[...] = jnp.zeros_like(values_ref)

    sums = dot_f32(normed_ref[...], w_ref[...], ((1,), (0,)))
    chunk = WINDOW
    wide = 2 * HEAD
    lane = lax.broadcasted_iota(jnp.int32, (chunk, wide), 1)
    sink = sink_ref[0]
    drive_high, drive_low = split_halves(drive_ref[...])
    out_high, out_low = split_halves(out_ref[...])
    powers = [(pole_ref[0, 0:1, :], pole_ref[0, 1:2, :])]
    while 2 ** len(powers) < chunk:
        powers.append(complex_mul(*powers[-1], *powers[-1]))
    old_keys, old_values = (keys_ref[...], values_ref[...])
    carry_re, carry_im = (carry_ref[0:1, :], carry_ref[1:2, :])
    for at in range(0, sums.shape[0], chunk):
        turned = sums[at : at + chunk, :wide]
        swapped = jnp.where(
            lane % HEAD < HEAD // 2,
            pltpu.roll(turned, wide - HEAD // 2, 1),
            pltpu.roll(turned, HEAD // 2, 1),
        )
        turned = turned * cosine_ref[at : at + chunk] + swapped * sine_ref[at : at + chunk]
        queries = jnp.where(lane < HEAD, turned, 0.0).astype(jnp.bfloat16)
        keys = pltpu.roll(turned, HEAD, 1).astype(jnp.bfloat16)
        values = sums[at : at + chunk, wide:].astype(jnp.bfloat16)
        attended = attend(
            queries, keys, values, old_keys, old_values, sink, start if at == 0 else None
        )
        old_keys, old_values = (keys, values)
        plain = ((1,), (0,))
        pushed = dot_f32(values, drive_high, plain) + dot_f32(values, drive_low, plain)
        half = pushed.shape[1] // 2
        re, im = (pushed[:, :half], pushed[:, half:])
        add_re, add_im = complex_mul(carry_re, carry_im, *powers[0])
        first = lax.broadcasted_iota(jnp.int32, re.shape, 0) == 0
        re = re + jnp.where(first, add_re, 0.0)
        im = im + jnp.where(first, add_im, 0.0)
        for level, power in enumerate(powers):
            move_re, move_im = complex_mul(
                shifted(re, 2**level), shifted(im, 2**level), *power
            )
            re, im = (re + move_re, im + move_im)
        carry_re, carry_im = (re[chunk - 1 :], im[chunk - 1 :])
        state_high, state_low = split_halves(jnp.concatenate([re, im], axis=1))
        contract = ((1,), (1,))
        summed = (
            dot_f32(state_high, out_high, contract)
            + dot_f32(state_low, out_high, contract)
            + dot_f32(state_high, out_low, contract)
        )
        mixed = jax.nn.gelu(summed + skip_ref[...] * values.astype(jnp.float32))
        acts_ref[at : at + chunk, :] = jnp.where(lane < HEAD, attended, mixed).astype(
            jnp.bfloat16
        )
    keys_ref[...] = old_keys
    values_ref[...] = old_values
    carry_ref[0:1, :] = carry_re
    carry_ref[1:2, :] = carry_im


def layer(normed, w_in, cosine, sine, sink_logit, poles, drive, readout, skip_gain):
    rows, depth = normed.shape
    block = math.gcd(rows, 4 * WINDOW)
    wide = 2 * HEAD
    states = poles.shape[2]

    def whole(value):
        return pl.BlockSpec(value.shape, lambda t: (0,) * value.ndim)

    def by_rows(width):
        return pl.BlockSpec((block, width), lambda t: (t, 0))

    front = ((wide - drive.shape[1], 0), (0, 0))
    drive = jnp.pad(drive[0], front)
    readout = jnp.pad(readout[0], front)
    skip = jnp.pad(skip_gain, front[0]).reshape(1, wide)
    return pl.pallas_call(
        layer_kernel,
        grid=(rows // block,),
        in_specs=[
            pl.BlockSpec(memory_space=pltpu.SMEM),
            by_rows(depth),
            whole(w_in),
            by_rows(wide),
            by_rows(wide),
            whole(drive),
            whole(poles),
            whole(readout),
            whole(skip),
        ],
        out_specs=by_rows(wide),
        out_shape=jax.ShapeDtypeStruct((rows, wide), jnp.bfloat16),
        scratch_shapes=[
            pltpu.VMEM((WINDOW, wide), jnp.bfloat16),
            pltpu.VMEM((WINDOW, wide), jnp.bfloat16),
            pltpu.VMEM((2, states), jnp.float32),
        ],
    )(sink_logit, normed, w_in, cosine, sine, drive, poles, readout, skip)


def out_kernel(acts_ref, w_ref, sum_ref):
    cores = w_ref.shape[0]
    total = None
    for core in range(cores):
        rows = jnp.concatenate(
            [acts_ref[at] for at in range(core, acts_ref.shape[0], cores)], axis=1
        )
        piece = dot_f32(rows, w_ref[core], ((1,), (0,)))
        piece = piece.astype(jnp.bfloat16).astype(jnp.float32)
        total = piece if total is None else total + piece
    sum_ref[...] = total.astype(jnp.bfloat16)


def out_project(acts, w_pair):
    devices, rows, width = acts.shape
    cores, depth, columns = w_pair.shape
    block = math.gcd(rows, 256)
    return pl.pallas_call(
        out_kernel,
        grid=(rows // block,),
        in_specs=[
            pl.BlockSpec((devices, block, width), lambda t: (0, t, 0)),
            pl.BlockSpec((cores, depth, columns), lambda t: (0, 0, 0)),
        ],
        out_specs=pl.BlockSpec((block, columns), lambda t: (t, 0)),
        out_shape=jax.ShapeDtypeStruct((rows, columns), jnp.bfloat16),
    )(acts, w_pair)


def own_part(value, axis_name):
    size = value.shape[0] // lax.axis_size(axis_name)
    return lax.dynamic_slice_in_dim(value, lax.axis_index(axis_name) * size, size, 0)


def normalize(tokens, norm_gain):
    wide_tokens = tokens.astype(jnp.float32)
    return (
        wide_tokens
        * lax.rsqrt(jnp.mean(wide_tokens * wide_tokens, axis=-1, keepdims=True) + epsilon)
        * norm_gain
    ).astype(jnp.bfloat16)


def by_heads(
    tokens,
    norm_gain,
    w_query,
    w_key,
    w_value,
    w_state_in,
    sink_logit,
    decay_rate,
    rotation,
    log_step,
    in_re,
    in_im,
    out_re,
    out_im,
    skip_gain,
    w_attn_out,
    w_state_out,
    out_gain,
):
    devices = lax.axis_size("sp")
    row_count = tokens.shape[0]
    everyone = ("sp", "tp")
    normed = lax.all_gather(
        normalize(own_part(tokens, "tp"), norm_gain), everyone, axis=0, tiled=True
    )
    rows = normed.shape[0]
    depth = w_query.shape[0]
    repeats = devices // (w_key.shape[1] // HEAD)

    def per_device(weight):
        return weight.reshape(depth, devices, weight.shape[1] // devices)

    def per_head(weight):
        return jnp.repeat(weight.reshape(depth, -1, HEAD), repeats, axis=1)

    pieces = (per_device(w_query), per_head(w_key), per_head(w_value), per_device(w_state_in))
    parcels = jnp.concatenate(pieces, axis=2).transpose(1, 0, 2)
    w_in = lax.all_to_all(parcels, "sp", split_axis=0, concat_axis=0, tiled=True)
    w_in = w_in.reshape(devices * depth, parcels.shape[2])

    def rows_of(weight):
        return weight.reshape(devices, weight.shape[0] // devices, weight.shape[1])

    w_out = jnp.concatenate([rows_of(w_attn_out), rows_of(w_state_out)], axis=1)
    w_out = w_out.reshape(1, -1, w_out.shape[2])
    w_pair = lax.all_to_all(w_out, "tp", split_axis=2, concat_axis=0, tiled=True)
    decay_rate, rotation, log_step, in_re, in_im, out_re, out_im, skip_gain, sink_logit = [
        own_part(value, "sp")
        for value in (
            decay_rate, rotation, log_step, in_re, in_im, out_re, out_im, skip_gain, sink_logit
        )
    ]
    poles, drive, readout = state_params(
        decay_rate, rotation, log_step, in_re, in_im, out_re, out_im
    )
    frequency = rotary_base ** (-(jnp.arange(HEAD // 2, dtype=jnp.float32) * 2.0 / HEAD))
    angles = jnp.arange(rows, dtype=jnp.int32).astype(jnp.float32)[:, None] * frequency[None, :]
    sine_part = jnp.sin(angles)
    cosine = jnp.tile(jnp.cos(angles), (1, 4))
    sine = jnp.concatenate([-sine_part, sine_part, -sine_part, sine_part], axis=1)
    mine = layer(normed, w_in, cosine, sine, sink_logit, poles, drive, readout, skip_gain)
    acts = lax.all_gather(mine, everyone, axis=0, tiled=False)
    summed = out_project(acts, w_pair)
    projected = lax.all_to_all(summed, everyone, split_axis=0, concat_axis=1, tiled=True)
    projected = projected.astype(jnp.float32)
    row_scale = lax.rsqrt(jnp.mean(projected * projected, axis=-1, keepdims=True) + epsilon)
    return (projected * row_scale * out_gain).astype(jnp.bfloat16)


def everyones(value, axis):
    size = lax.axis_size(axis)
    copies = jnp.broadcast_to(value[None], (size,) + value.shape)
    return lax.all_to_all(copies, axis, split_axis=0, concat_axis=0, tiled=True)


def earlier_window(key_rows, value_rows):
    joined = jnp.concatenate([key_rows, value_rows], axis=1)
    prior = passed_along(joined, "sp", 1)
    return jnp.concatenate([prior, joined], axis=0)


def by_tokens(
    tokens,
    norm_gain,
    w_query,
    w_key,
    w_value,
    w_state_in,
    sink_logit,
    decay_rate,
    rotation,
    log_step,
    in_re,
    in_im,
    out_re,
    out_im,
    skip_gain,
    w_attn_out,
    w_state_out,
    out_gain,
):
    row_count = tokens.shape[0]
    window = WINDOW
    head_width = HEAD
    wide_tokens = tokens.astype(jnp.float32)
    normed = (
        wide_tokens
        * lax.rsqrt(jnp.mean(wide_tokens * wide_tokens, axis=-1, keepdims=True) + epsilon)
        * norm_gain
    ).astype(jnp.bfloat16)
    first_row = lax.axis_index("sp") * row_count
    positions = first_row + jnp.arange(row_count, dtype=jnp.int32)
    poles, drive, readout = state_params(
        decay_rate, rotation, log_step, in_re, in_im, out_re, out_im
    )
    slab = lax.all_to_all(normed, "sp", split_axis=1, concat_axis=0, tiled=True)
    w_in = jnp.concatenate([w_query, w_key, w_value, w_state_in], axis=1)
    sums = lax.psum_scatter(
        jnp.dot(slab, w_in, preferred_element_type=jnp.float32).astype(jnp.bfloat16),
        "sp",
        scatter_dimension=0,
        tiled=True,
    )
    key_at = w_query.shape[1]
    value_at = key_at + w_key.shape[1]
    input_at = value_at + w_value.shape[1]
    inputs = sums[:, input_at:]
    ends = everyones(state_ends(inputs, poles, drive), "sp")
    queries, key_rows, value_rows = shape_heads(
        sums[:, :key_at].astype(jnp.float32),
        sums[:, key_at:value_at].astype(jnp.float32),
        sums[:, value_at:input_at],
        positions,
        head_width,
    )
    joined_rows = earlier_window(key_rows, value_rows)
    kv_width = key_rows.shape[1]
    kv_heads = kv_width // head_width
    all_keys = joined_rows[:, :kv_width].reshape(window + row_count, kv_heads, head_width)
    all_values = joined_rows[:, kv_width:].reshape(window + row_count, kv_heads, head_width)
    attended = band_attention(queries, all_keys, all_values, sink_logit, first_row, window)
    mixed_state = state_mix(inputs, poles, drive, readout, ends, skip_gain)
    rows = lax.all_gather(
        jnp.concatenate([attended, mixed_state], axis=1), "sp", axis=0, tiled=True
    )
    w_out = jnp.concatenate([w_attn_out, w_state_out], axis=0)
    partial = jnp.dot(rows, w_out, preferred_element_type=jnp.float32).astype(jnp.bfloat16)
    cores = lax.axis_size("tp")
    blocks = partial.reshape(-1, cores, row_count // cores, partial.shape[1])
    halves = lax.all_to_all(blocks, "tp", split_axis=1, concat_axis=1, tiled=True)
    summed = jnp.sum(halves.astype(jnp.float32), axis=1).astype(jnp.bfloat16)
    projected = lax.all_to_all(summed, "sp", split_axis=0, concat_axis=2, tiled=True)
    projected = projected.reshape(row_count // cores, -1).astype(jnp.float32)
    row_scale = lax.rsqrt(jnp.mean(projected * projected, axis=-1, keepdims=True) + epsilon)
    return (projected * row_scale * out_gain).astype(jnp.bfloat16)


def body(tokens, norm_gain, w_query, w_key, *others):
    devices = lax.axis_size("sp")
    heads = w_query.shape[1] // HEAD
    groups = others[5].shape[0]
    fits = (
        heads == devices
        and groups % devices == 0
        and others[1].shape[1] == w_query.shape[1]
        and tokens.shape[0] % WINDOW == 0
        and tokens.shape[0] % (8 * lax.axis_size("tp")) == 0
    )
    return (by_heads if fits else by_tokens)(tokens, norm_gain, w_query, w_key, *others)


def solution(mesh):
    return jax.shard_map(
        body,
        mesh=mesh,
        in_specs=(
            P("sp", None),
            P(),
            P("sp", "tp"),
            P("sp", "tp"),
            P("sp", "tp"),
            P("sp", "tp"),
            P("tp"),
            P("tp", None),
            P("tp", None),
            P("tp"),
            P("tp", None, None),
            P("tp", None, None),
            P("tp", None, None),
            P("tp", None, None),
            P("tp"),
            P("tp", "sp"),
            P("tp", "sp"),
            P(),
        ),
        out_specs=P(("sp", "tp"), None),
        check_vma=False,
    )
```
